32 devices in a mesh: fs: 4 (over y, x), tp: 8 (over z, core).
Axes of the slice: x: 2, y: 2, z: 4, core: 2. Of those that a mesh axis runs over, the one named last changes fastest.
Arguments:
- inputs: bfloat16 [8, 320, 2048], P('tp'), may hold values from -6 to 6
- cotangent: bfloat16 [8, 320, 2048], P('tp'), may hold values from -8 to 8
- gate_weight: bfloat16 [2048, 5632], P('tp', 'fs'), may hold values from -0.125 to 0.125
- up_weight: bfloat16 [2048, 5632], P('tp', 'fs'), may hold values from -0.125 to 0.125
- down_weight: bfloat16 [5632, 2048], P('fs', 'tp'), may hold values from -0.078125 to 0.078125
Outputs:
- input_grad: bfloat16 [8, 320, 2048], P('tp')
- down_grad: float32 [5632, 2048], P('fs', 'tp')
The draws below stay inside these ranges and needn't reach their ends.
All inputs are finite; a program needn't handle non-finite values.
Results may differ from the reference program's by a relative error of at most 0.023.
Values may be sent and summed in bfloat16 or wider, within the bound.
A program may use at most 64 MiB of HBM per device.

```python
import jax
import jax.numpy as jnp
from jax import lax

D = 2048
FF = 5632
TOK_DEV = 320
SPANS = 8
N_FS = 4


def spiked(array, key, source, target, shards_of, factor):
    def block_of(position):
        return (jnp.arange(array.shape[position]) // (array.shape[position] // shards_of)).reshape((-1,) + (1,) * (array.ndim - 1 - position))

    first = jax.random.permutation(key, shards_of)[block_of(target)]
    other_side = (block_of(target) + shards_of // 2) % shards_of
    return jnp.where((block_of(source) == first) | (block_of(source) == other_side), factor * array, array)


def levels(rng, shape, cuts, low, high):
    loudness, own = 1.0, jax.random.fold_in(rng, 6)
    for position, blocks in cuts:
        heights = jnp.exp(jax.random.uniform(jax.random.fold_in(own, position), (blocks,), jnp.float32, low / len(cuts), high / len(cuts)))
        loudness = loudness * jnp.repeat(heights, shape[position] // blocks).reshape([-1 if axis == position else 1 for axis in range(len(shape))])
    return loudness


def centred(stream_key, extent, scale, limit, cuts=(), dtype=jnp.bfloat16):
    values = scale * jax.random.normal(stream_key, extent, jnp.float32)
    if cuts:
        values = values * levels(stream_key, extent, cuts, -0.22, 0.18)
    return jnp.clip(values, -limit, limit).astype(dtype)


def noise_with(own_key, extent, scale, limit, cuts, heavy, kind=jnp.bfloat16):
    array = scale * jax.random.normal(own_key, extent, jnp.float32)
    if cuts:
        array = array * levels(own_key, extent, cuts, -0.22, 0.18)
    return jnp.clip(spiked(array, jax.random.fold_in(own_key, 3), *heavy), -limit, limit).astype(kind)


def setup_inputs(seed: int = 0) -> dict:
    splits = jax.random.split(jax.random.key(seed), 6)
    inputs = centred(splits[0], (SPANS, TOK_DEV, D), 1.0, 6.0, ((0, 8),))
    cotangent = noise_with(splits[1], (SPANS, TOK_DEV, D), 1.0, 8.0, ((0, 8),), (0, 2, 8, 2.0))
    gate_weight = centred(splits[2], (D, FF), D ** -0.5, 0.125, ((0, 8), (1, 4)))
    up_weight = centred(splits[3], (D, FF), D ** -0.5, 0.125, ((0, 8), (1, 4)))
    down_weight = centred(splits[4], (FF, D), FF ** -0.5, 0.078125, ((0, 4), (1, 8)))
    return {"inputs": inputs, "cotangent": cotangent, "gate_weight": gate_weight, "up_weight": up_weight, "down_weight": down_weight}


def reference(inputs, cotangent, gate_weight, up_weight, down_weight):
    rows_in = inputs.reshape(-1, D)
    rows_grad = cotangent.reshape(-1, D)
    gate_pre = jnp.dot(rows_in, gate_weight, preferred_element_type=jnp.float32)
    up_pre = jnp.dot(rows_in, up_weight, preferred_element_type=jnp.float32)
    sig = jax.nn.sigmoid(gate_pre)
    hidden = (gate_pre * sig * up_pre).astype(jnp.bfloat16)
    down_grad = jnp.dot(hidden.T, rows_grad, preferred_element_type=jnp.float32)
    hidden_grad = jnp.dot(rows_grad, down_weight.T, preferred_element_type=jnp.float32)
    gate_grad = (hidden_grad * up_pre * sig * (1.0 + gate_pre * (1.0 - sig))).astype(jnp.bfloat16)
    up_grad = (hidden_grad * gate_pre * sig).astype(jnp.bfloat16)
    width = FF // N_FS
    total_rows = rows_in.shape[0]
    gate_blocks = gate_weight.reshape(D, N_FS, width).transpose(1, 0, 2)
    up_blocks = up_weight.reshape(D, N_FS, width).transpose(1, 0, 2)
    gate_cols = gate_grad.reshape(total_rows, N_FS, width).transpose(1, 0, 2)
    up_cols = up_grad.reshape(total_rows, N_FS, width).transpose(1, 0, 2)

    def add_block(total, pieces):
        g_weight, u_weight, g_cols, u_cols = pieces
        term = jnp.dot(g_cols, g_weight.T, preferred_element_type=jnp.float32)
        term = term + jnp.dot(u_cols, u_weight.T, preferred_element_type=jnp.float32)
        return total + term.astype(jnp.bfloat16).astype(jnp.float32), None

    start_total = jnp.zeros((total_rows, D), jnp.float32)
    total, unused = lax.scan(add_block, start_total, (gate_blocks, up_blocks, gate_cols, up_cols))
    input_grad = total.astype(jnp.bfloat16).reshape(inputs.shape)
    return input_grad, down_grad
```

```python
import functools

import jax
import jax.numpy as jnp
from jax import lax
from jax.experimental import pallas as pl
from jax.experimental.pallas import tpu as pltpu
from jax.sharding import PartitionSpec as P

MESH = pl.DeviceIdType.MESH
BF16 = jnp.bfloat16
F32 = jnp.float32


def contract_hidden(left, right):
    return lax.dot_general(left, right, (((1,), (1,)), ((), ())), preferred_element_type=F32)


def contract_tokens(left, right):
    return lax.dot_general(left, right, (((0,), (0,)), ((), ())), preferred_element_type=F32)


def gathered(inputs, cotangent, gate_weight, up_weight, down_weight):
    rows_in = inputs[0]
    rows_grad = cotangent[0]
    token_count, model_width = rows_in.shape
    gate_full = lax.all_gather(gate_weight, "tp", axis=0, tiled=True)
    up_full = lax.all_gather(up_weight, "tp", axis=0, tiled=True)
    down_tall = lax.all_gather(down_weight.T, "tp", axis=0, tiled=True)
    gate_pre = jnp.dot(rows_in, gate_full, preferred_element_type=F32)
    up_pre = jnp.dot(rows_in, up_full, preferred_element_type=F32)
    sig = jax.nn.sigmoid(gate_pre)
    hidden = (gate_pre * sig * up_pre).astype(BF16)
    hidden_grad = jnp.dot(rows_grad, down_tall, preferred_element_type=F32)
    gate_grad = (hidden_grad * up_pre * sig * (1.0 + gate_pre * (1.0 - sig))).astype(BF16)
    up_grad = (hidden_grad * gate_pre * sig).astype(BF16)
    partial_down = contract_tokens(hidden, rows_grad)
    down_grad = lax.psum_scatter(
        partial_down.astype(BF16), "tp", scatter_dimension=1, tiled=True
    ).astype(F32)
    own_sum = lax.psum_scatter(
        (contract_hidden(gate_grad, gate_full) + contract_hidden(up_grad, up_full)).astype(BF16),
        "fs",
        scatter_dimension=0,
        tiled=True,
    )
    whole_grad = lax.all_gather(own_sum, "fs", axis=0, tiled=True)
    return (whole_grad.reshape(1, token_count, model_width), down_grad)


def kernel(
    n_tp, x_ref, ct_ref, wg_ref, wu_ref, wd_ref, grad_ref, down_ref,
    tok, part, core_in, half_in, quarter_in, chain_in, wts, acc, down_out, down_in,
    loc_sem, tok_rs, z_ss, xy_ss, dg_ss, d2d_ss, d2d_rs, w_ss, w_rs, core_ss, core_rs,
    half_ss, half_rs, q_ss, q_rs, ch_ss, ch_rs, ag_ss, ag_rs, dn_ss, dn_rs,
):
    f, t = lax.axis_index("fs"), lax.axis_index("tp")
    n_z = n_tp // 2
    z, c = t // 2, t % 2
    fy, fx = f // 2, f % 2
    f_x = fy * 2 + (1 - fx)
    f_y = (1 - fy) * 2 + fx
    f_d = (1 - fy) * 2 + (1 - fx)
    dev_x, dev_y, dev_d = {"fs": f_x}, {"fs": f_y}, {"fs": f_d}
    partner = {"tp": z * 2 + (1 - c)}
    n_tok, width = tok.shape[2], tok.shape[3]
    qr = n_tok // 4
    hid = wts.shape[1]
    cols = width // n_tp

    def plane(delta):
        return {"tp": (z + delta) * 2 + c}

    def rc(src, dst, ss, rs, dev):
        return pltpu.make_async_remote_copy(
            src_ref=src, dst_ref=dst, send_sem=ss, recv_sem=rs, device_id=dev, device_id_type=MESH
        )

    def qs(q):
        return pl.ds(pl.multiple_of(q * qr, qr), qr)

    def tokq(arr, span, q):
        return tok.at[arr, span, qs(q)]

    own = [
        pltpu.make_async_copy(x_ref.at[0], tok.at[0, t], loc_sem.at[0]),
        pltpu.make_async_copy(ct_ref.at[0], tok.at[1, t], loc_sem.at[1]),
    ]
    own_cols = pl.ds(pl.multiple_of(t * cols, cols), cols)
    for i, w in enumerate((wg_ref, wu_ref, wd_ref)):
        own.append(
            pltpu.make_async_copy(
                w.at[pl.ds(pl.multiple_of(t * hid, hid), hid)], wts.at[i, :, own_cols], loc_sem.at[2 + i]
            )
        )
    for copy in own:
        copy.start()

    barrier = pltpu.get_barrier_semaphore()
    for dev in (dev_x, dev_y, dev_d):
        pl.semaphore_signal(barrier, inc=1, device_id=dev, device_id_type=MESH)
    for k in range(1, n_tp):
        pl.semaphore_signal(barrier, inc=1, device_id={"tp": (t + k) % n_tp}, device_id_type=MESH)
    pl.semaphore_wait(barrier, 3 + n_tp - 1)
    for copy in own:
        copy.wait()

    def z_copy(arr, p, d):
        src = tokq(arr, p * 2 + c, f)
        return rc(src, src, z_ss.at[arr, p, d], tok_rs.at[arr, p, f], plane(1 if d else -1))

    def xy_copy(arr, p, d):
        src = tokq(arr, p * 2 + c, f)
        return rc(src, src, xy_ss.at[arr, p, d], tok_rs.at[arr, p, f], dev_y if d else dev_x)

    def relay_copy(arr, p):
        q = f_y if arr else f_x
        src = tokq(arr, p * 2 + c, q)
        return rc(src, src, dg_ss.at[arr, p], tok_rs.at[arr, p, q], dev_x if arr else dev_y)

    def tok_wait(arr, p, q):
        dst = tokq(arr, p * 2 + c, q)
        rc(dst, dst, z_ss.at[arr, p, 0], tok_rs.at[arr, p, q], dev_x).wait_recv()

    def d2d_copy(arr, p, core):
        src = tok.at[arr, p * 2 + core]
        return rc(src, src, d2d_ss.at[arr, p], d2d_rs.at[arr, p], partner)

    def w_copy(i, k):
        to = (t + k) % n_tp
        return rc(
            (wg_ref, wu_ref, wd_ref)[i].at[pl.ds(pl.multiple_of(to * hid, hid), hid)],
            wts.at[i, :, own_cols], w_ss.at[i, k], w_rs.at[i, k], {"tp": to},
        )

    for arr in range(2):
        for d, ok in ((1, z < n_z - 1), (0, z > 0)):
            @pl.when(ok)
            def _(arr=arr, d=d):
                z_copy(arr, z, d).start()
        d2d_copy(arr, z, c).start()

    w_order = list(range(1, n_tp))
    for step in range(1, n_z):
        for i in range(3):
            for k in w_order[(step - 1) * len(w_order) // (n_z - 1):step * len(w_order) // (n_z - 1)]:
                w_copy(i, k).start()
        for d in (1, 0):
            p = z - step if d else z + step

            @pl.when((p >= 0) & (p < n_z))
            def _(p=p, d=d):
                for arr in range(2):
                    tok_wait(arr, p, f)

                    @pl.when(z < n_z - 1 if d else z > 0)
                    def _():
                        z_copy(arr, p, d).start()

                    xy_copy(arr, p, 0).start()
                    xy_copy(arr, p, 1).start()

    def order(j):
        return jnp.where(z < n_z // 2, z + j, z - j + n_z) % n_z

    @pl.loop(1, n_z)
    def _(j):
        p = order(j)
        tok_wait(0, p, f_x)
        relay_copy(0, p).start()
        tok_wait(1, p, f_y)
        relay_copy(1, p).start()

    @pl.loop(1, n_z)
    def _(j):
        p = order(j)
        tok_wait(0, p, f_y)
        tok_wait(0, p, f_d)
        d2d_copy(0, p, c).start()
        tok_wait(1, p, f_x)
        tok_wait(1, p, f_d)
        d2d_copy(1, p, c).start()

    for i in range(3):
        for k in range(1, n_tp):
            frm = (t - k + n_tp) % n_tp
            dst = wts.at[i, :, pl.ds(pl.multiple_of(frm * cols, cols), cols)]
            rc(dst, dst, w_ss.at[i, k], w_rs.at[i, k], partner).wait_recv()

    acc[...] = jnp.zeros_like(acc)

    def core_copy(p):
        return rc(part.at[p * 2 + 1 - c], core_in.at[p], core_ss.at[p], core_rs.at[p], partner)

    def half_copy(p, first_x, i):
        q = jnp.where(first_x, i * 2 + (1 - fx), (1 - fy) * 2 + i)
        dev = {"fs": jnp.where(first_x, f_x, f_y)}
        return rc(part.at[p * 2 + c, qs(q)], half_in.at[p, i], half_ss.at[p, i], half_rs.at[p, i], dev)

    @pl.loop(0, n_z)
    def _(j):
        p = order(j)
        for arr in range(2):
            dst = tok.at[arr, p * 2 + 1 - c]
            rc(dst, dst, d2d_ss.at[arr, p], d2d_rs.at[arr, p], partner).wait_recv()

        @pl.loop(0, 2)
        def _(u):
            s = p * 2 + jnp.where(u == 0, 1 - c, c)
            rows, ct = tok[0, s], tok[1, s]
            gate_pre = contract_hidden(rows, wts[0])
            up_pre = contract_hidden(rows, wts[1])
            hidden_grad = contract_hidden(ct, wts[2])
            sig = jax.nn.sigmoid(gate_pre)
            silu = gate_pre * sig
            hidden = (silu * up_pre).astype(BF16)
            gate_grad = (hidden_grad * up_pre * sig * (1.0 + gate_pre * (1.0 - sig))).astype(BF16)
            up_grad = (hidden_grad * silu).astype(BF16)
            acc[...] += contract_tokens(hidden, ct)
            part[s] = (
                jnp.dot(gate_grad, wts[0], preferred_element_type=F32)
                + jnp.dot(up_grad, wts[1], preferred_element_type=F32)
            ).astype(BF16)

            @pl.when(u == 0)
            def _():
                core_copy(p).start()

        core_copy(p).wait_recv()
        s = p * 2 + c
        part[s] = (part[s].astype(F32) + core_in[p].astype(F32)).astype(BF16)
        first_x = p % 2 == 0
        half_copy(p, first_x, 0).start()
        half_copy(p, first_x, 1).start()

    down_out[...] = acc[...].astype(BF16)

    def dn_copy(k):
        to = (t + k) % n_tp
        return rc(
            down_out.at[:, pl.ds(pl.multiple_of(to * cols, cols), cols)],
            down_in.at[pl.ds(pl.multiple_of(t * hid, hid), hid)],
            dn_ss.at[k], dn_rs.at[k], {"tp": to},
        )

    for k in range(1, n_tp):
        dn_copy(k).start()

    def quarter_copy(p, first_x):
        q = jnp.where(first_x, f_y, f_x)
        return rc(
            part.at[p * 2 + c, qs(q)], quarter_in.at[p], q_ss.at[p], q_rs.at[p],
            {"fs": jnp.where(first_x, f_y, f_x)},
        )

    @pl.loop(0, n_z)
    def _(j):
        p = order(j)
        first_x = p % 2 == 0
        s = p * 2 + c
        other = jnp.where(first_x, 1 - fy, 1 - fx)
        mine = jnp.where(first_x, fy, fx)
        for i in range(2):
            half_copy(p, first_x, i).wait_recv()
        q_other = jnp.where(first_x, f_y, f_x)
        part[s, qs(q_other)] = (
            part[s, qs(q_other)].astype(F32) + half_in[p, other].astype(F32)
        ).astype(BF16)
        quarter_copy(p, first_x).start()
        part[s, qs(f)] = (part[s, qs(f)].astype(F32) + half_in[p, mine].astype(F32)).astype(BF16)

    @pl.loop(0, n_z)
    def _(j):
        p = order(j)
        quarter_copy(p, p % 2 == 0).wait_recv()
        s = p * 2 + c
        part[s, qs(f)] = (part[s, qs(f)].astype(F32) + quarter_in[p].astype(F32)).astype(BF16)

    def chain_copy(p, d):
        return rc(
            part.at[p * 2 + c, qs(f)], chain_in.at[p, d], ch_ss.at[p], ch_rs.at[p, d],
            plane(1 if d else -1),
        )

    def chain_add(p, d):
        chain_copy(p, d).wait_recv()
        s = p * 2 + c
        part[s, qs(f)] = (part[s, qs(f)].astype(F32) + chain_in[p, d].astype(F32)).astype(BF16)

    for step in range(n_z - 1, 0, -1):
        for d in (1, 0):
            p = z + step if d else z - step

            @pl.when((p >= 0) & (p < n_z))
            def _(p=p, d=d):
                @pl.when(z > 0 if d else z < n_z - 1)
                def _():
                    chain_add(p, d)

                chain_copy(p, d).start()

    @pl.when(z > 0)
    def _():
        chain_add(z, 1)

    @pl.when(z < n_z - 1)
    def _():
        chain_add(z, 0)

    grad_ref[0, qs(f)] = part[t, qs(f)]

    def ag_copy(i, q):
        return rc(
            part.at[t, qs(f)], grad_ref.at[0, qs(q)], ag_ss.at[i], ag_rs.at[i], (dev_x, dev_y, dev_d)[i]
        )

    for i in (2, 0, 1):
        ag_copy(i, f).start()

    down_ref[pl.ds(pl.multiple_of(t * hid, hid), hid)] = acc[:, own_cols]
    for k in range(1, n_tp):
        frm = (t - k + n_tp) % n_tp
        rows = pl.ds(pl.multiple_of(frm * hid, hid), hid)
        rc(down_in.at[rows], down_in.at[rows], dn_ss.at[k], dn_rs.at[k], partner).wait_recv()
        down_ref[rows] = down_in[rows].astype(F32)

    for i, q in enumerate((f_x, f_y, f_d)):
        ag_copy(i, q).wait_recv()

    for arr in range(2):
        for p in range(n_z):
            @pl.when((z < n_z - 1) & (p <= z))
            def _(arr=arr, p=p):
                z_copy(arr, p, 1).wait_send()

            @pl.when((z > 0) & (p >= z))
            def _(arr=arr, p=p):
                z_copy(arr, p, 0).wait_send()

            d2d_copy(arr, p, c).wait_send()

            @pl.when(p != z)
            def _(arr=arr, p=p):
                xy_copy(arr, p, 0).wait_send()
                xy_copy(arr, p, 1).wait_send()
                relay_copy(arr, p).wait_send()

    for k in range(1, n_tp):
        for i in range(3):
            w_copy(i, k).wait_send()
        dn_copy(k).wait_send()
    for p in range(n_z):
        core_copy(p).wait_send()
        half_copy(p, p % 2 == 0, 0).wait_send()
        half_copy(p, p % 2 == 0, 1).wait_send()
        quarter_copy(p, p % 2 == 0).wait_send()

        @pl.when(p != z)
        def _(p=p):
            chain_copy(p, 0).wait_send()

    for i in range(3):
        ag_copy(i, f).wait_send()


def spread(n_tp, inputs, cotangent, gate_weight, up_weight, down_weight):
    _, n_tok, width = inputs.shape
    hid_all = gate_weight.shape[1]
    hid, cols, n_z, qr = hid_all // n_tp, width // n_tp, n_tp // 2, n_tok // 4
    dma = pltpu.SemaphoreType.DMA
    vmem = pl.BlockSpec(memory_space=pltpu.VMEM)
    anyspace = pl.BlockSpec(memory_space=pl.ANY)
    return pl.pallas_call(
        functools.partial(kernel, n_tp),
        name="spread_hidden",
        out_shape=(
            jax.ShapeDtypeStruct((1, n_tok, width), BF16),
            jax.ShapeDtypeStruct((hid_all, cols), F32),
        ),
        in_specs=[anyspace, anyspace, vmem, vmem, vmem],
        out_specs=(vmem, vmem),
        scratch_shapes=[
            pltpu.VMEM((2, n_tp, n_tok, width), BF16),
            pltpu.VMEM((n_tp, n_tok, width), BF16),
            pltpu.VMEM((n_z, n_tok, width), BF16),
            pltpu.VMEM((n_z, 2, qr, width), BF16),
            pltpu.VMEM((n_z, qr, width), BF16),
            pltpu.VMEM((n_z, 2, qr, width), BF16),
            pltpu.VMEM((3, hid, width), BF16),
            pltpu.VMEM((hid, width), F32),
            pltpu.VMEM((hid, width), BF16),
            pltpu.VMEM((hid_all, cols), BF16),
            dma((5,)), dma((2, n_z, 4)), dma((2, n_z, 2)), dma((2, n_z, 2)), dma((2, n_z)),
            dma((2, n_z)), dma((2, n_z)), dma((3, n_tp)), dma((3, n_tp)), dma((n_z,)), dma((n_z,)),
            dma((n_z, 2)), dma((n_z, 2)), dma((n_z,)), dma((n_z,)), dma((n_z,)), dma((n_z, 2)),
            dma((3,)), dma((3,)), dma((n_tp,)), dma((n_tp,)),
        ],
        compiler_params=pltpu.CompilerParams(
            collective_id=0, has_side_effects=True, vmem_limit_bytes=66_000_000
        ),
    )(inputs, cotangent, gate_weight.T, up_weight.T, down_weight)


def solution(mesh):
    n_fs, n_tp = mesh.shape["fs"], mesh.shape["tp"]

    def per_device(inputs, cotangent, gate_weight, up_weight, down_weight):
        _, n_tok, width = inputs.shape
        hid_all = gate_weight.shape[1]
        n_z = n_tp // 2
        fits = (
            n_fs == 4
            and n_tp % 2 == 0
            and hid_all % (n_tp * 16) == 0
            and width % (n_tp * 128) == 0
            and n_tok % 64 == 0
            and 2 * n_tok * width * (3 * n_tp + 3 * n_z + 4) + 16 * hid_all * width < 62_000_000 * 2
        )
        if not fits:
            return gathered(inputs, cotangent, gate_weight, up_weight, down_weight)
        return spread(n_tp, inputs, cotangent, gate_weight, up_weight, down_weight)

    return jax.shard_map(
        per_device,
        mesh=mesh,
        in_specs=(
            P("tp", None, None),
            P("tp", None, None),
            P("tp", "fs"),
            P("tp", "fs"),
            P("fs", "tp"),
        ),
        out_specs=(P("tp", None, None), P("fs", "tp")),
        check_vma=False,
    )
```

```python
import functools

import jax
import jax.numpy as jnp
from jax import lax
from jax.experimental import pallas as pl
from jax.experimental.pallas import tpu as pltpu
from jax.sharding import PartitionSpec as P

MESH = pl.DeviceIdType.MESH
BF16 = jnp.bfloat16
F32 = jnp.float32


def contract_hidden(left, right):
    return lax.dot_general(left, right, (((1,), (1,)), ((), ())), preferred_element_type=F32)


def contract_tokens(left, right):
    return lax.dot_general(left, right, (((0,), (0,)), ((), ())), preferred_element_type=F32)


def gathered(inputs, cotangent, gate_weight, up_weight, down_weight):
    rows_in = inputs[0]
    rows_grad = cotangent[0]
    token_count, model_width = rows_in.shape
    gate_full = lax.all_gather(gate_weight, "tp", axis=0, tiled=True)
    up_full = lax.all_gather(up_weight, "tp", axis=0, tiled=True)
    down_tall = lax.all_gather(down_weight.T, "tp", axis=0, tiled=True)
    gate_pre = jnp.dot(rows_in, gate_full, preferred_element_type=F32)
    up_pre = jnp.dot(rows_in, up_full, preferred_element_type=F32)
    sig = jax.nn.sigmoid(gate_pre)
    hidden = (gate_pre * sig * up_pre).astype(BF16)
    hidden_grad = jnp.dot(rows_grad, down_tall, preferred_element_type=F32)
    gate_grad = (hidden_grad * up_pre * sig * (1.0 + gate_pre * (1.0 - sig))).astype(BF16)
    up_grad = (hidden_grad * gate_pre * sig).astype(BF16)
    partial_down = contract_tokens(hidden, rows_grad)
    down_grad = lax.psum_scatter(
        partial_down.astype(BF16), "tp", scatter_dimension=1, tiled=True
    ).astype(F32)
    own_sum = lax.psum_scatter(
        (contract_hidden(gate_grad, gate_full) + contract_hidden(up_grad, up_full)).astype(BF16),
        "fs",
        scatter_dimension=0,
        tiled=True,
    )
    whole_grad = lax.all_gather(own_sum, "fs", axis=0, tiled=True)
    return (whole_grad.reshape(1, token_count, model_width), down_grad)


def kernel(
    n_tp, x_ref, ct_ref, wg_ref, wu_ref, wd_ref, grad_ref, down_ref,
    tok, part, core_in, half_in, quarter_in, chain_in, wts, acc, down_out, down_in,
    gate_t, up_t, loc_sem, tok_rs, z_ss, xy_ss, dg_ss, d2d_ss, d2d_rs, w_ss, w_rs, core_ss, core_rs,
    half_ss, half_rs, q_ss, q_rs, ch_ss, ch_rs, ag_ss, ag_rs, dn_ss, dn_rs,
):
    f, t = lax.axis_index("fs"), lax.axis_index("tp")
    n_z = n_tp // 2
    z, c = t // 2, t % 2
    fy, fx = f // 2, f % 2
    f_x = fy * 2 + (1 - fx)
    f_y = (1 - fy) * 2 + fx
    f_d = (1 - fy) * 2 + (1 - fx)
    dev_x, dev_y, dev_d = {"fs": f_x}, {"fs": f_y}, {"fs": f_d}
    partner = {"tp": z * 2 + (1 - c)}
    n_tok, width = tok.shape[2], tok.shape[3]
    qr = n_tok // 4
    hid = wts.shape[1]
    cols = width // n_tp

    def plane(delta):
        return {"tp": (z + delta) * 2 + c}

    def rc(src, dst, ss, rs, dev):
        return pltpu.make_async_remote_copy(
            src_ref=src, dst_ref=dst, send_sem=ss, recv_sem=rs, device_id=dev, device_id_type=MESH
        )

    def qs(q):
        return pl.ds(pl.multiple_of(q * qr, qr), qr)

    def tokq(arr, span, q):
        return tok.at[arr, span, qs(q)]

    own = [
        pltpu.make_async_copy(x_ref.at[0], tok.at[0, t], loc_sem.at[0]),
        pltpu.make_async_copy(ct_ref.at[0], tok.at[1, t], loc_sem.at[1]),
    ]
    own_cols = pl.ds(pl.multiple_of(t * cols, cols), cols)
    for copy in own:
        copy.start()

    barrier = pltpu.get_barrier_semaphore()
    for dev in (dev_x, dev_y, dev_d):
        pl.semaphore_signal(barrier, inc=1, device_id=dev, device_id_type=MESH)
    for k in range(1, n_tp):
        pl.semaphore_signal(barrier, inc=1, device_id={"tp": (t + k) % n_tp}, device_id_type=MESH)
    pl.semaphore_wait(barrier, 3 + n_tp - 1)
    for copy in own:
        copy.wait()

    def z_copy(arr, p, d):
        src = tokq(arr, p * 2 + c, f)
        return rc(src, src, z_ss.at[arr, p, d], tok_rs.at[arr, p, f], plane(1 if d else -1))

    def xy_copy(arr, p, d):
        src = tokq(arr, p * 2 + c, f)
        return rc(src, src, xy_ss.at[arr, p, d], tok_rs.at[arr, p, f], dev_y if d else dev_x)

    def relay_copy(arr, p):
        q = f_y if arr else f_x
        src = tokq(arr, p * 2 + c, q)
        return rc(src, src, dg_ss.at[arr, p], tok_rs.at[arr, p, q], dev_x if arr else dev_y)

    def tok_wait(arr, p, q):
        dst = tokq(arr, p * 2 + c, q)
        rc(dst, dst, z_ss.at[arr, p, 0], tok_rs.at[arr, p, q], dev_x).wait_recv()

    def d2d_copy(arr, p, core):
        src = tok.at[arr, p * 2 + core]
        return rc(src, src, d2d_ss.at[arr, p], d2d_rs.at[arr, p], partner)

    def w_copy(i, to):
        return rc(
            (gate_t, up_t, wd_ref)[i].at[pl.ds(pl.multiple_of(to * hid, hid), hid)],
            wts.at[i, :, own_cols], w_ss.at[i, to], w_rs.at[i, t], {"tp": to},
        )

    def w_send(d):
        @pl.loop(2, 2 * n_z)
        def _(k):
            p = z + k // 2 if d else z - k // 2

            @pl.when((p >= 0) & (p < n_z))
            def _():
                for i in range(3):
                    w_copy(i, p * 2 + k % 2).start()

    for arr in range(2):
        for d, ok in ((1, z < n_z - 1), (0, z > 0)):
            @pl.when(ok)
            def _(arr=arr, d=d):
                z_copy(arr, z, d).start()
        d2d_copy(arr, z, c).start()

    gate_t[...] = wg_ref[...].T
    up_t[...] = wu_ref[...].T
    own_rows = pl.ds(pl.multiple_of(t * hid, hid), hid)
    for i, w in enumerate((gate_t, up_t, wd_ref)):
        wts[i, :, own_cols] = w[own_rows]

    for i in range(3):
        w_copy(i, z * 2 + 1 - c).start()

    for step in range(n_z):
        for d in (1, 0):
            p = z - step if d else z + step

            if step == 0:
                continue

            @pl.when((p >= 0) & (p < n_z))
            def _(p=p, d=d):
                for arr in range(2):
                    tok_wait(arr, p, f)

                    @pl.when(z < n_z - 1 if d else z > 0)
                    def _():
                        z_copy(arr, p, d).start()

                    xy_copy(arr, p, 0).start()
                    xy_copy(arr, p, 1).start()

        for d in (1, 0):
            @pl.when((z if d else n_z - 1 - z) == step)
            def _(d=d):
                w_send(d)

    def order(j):
        return jnp.where(z < n_z // 2, z + j, z - j + n_z) % n_z

    def sweep(j):
        return jnp.where(j % 2 == 0, n_z - 1 - j // 2, j // 2)

    @pl.loop(1, n_z)
    def _(j):
        p = order(j)
        tok_wait(0, p, f_x)
        relay_copy(0, p).start()
        tok_wait(1, p, f_y)
        relay_copy(1, p).start()

    @pl.loop(1, n_z)
    def _(j):
        p = order(j)
        tok_wait(0, p, f_y)
        tok_wait(0, p, f_d)
        d2d_copy(0, p, c).start()
        tok_wait(1, p, f_x)
        tok_wait(1, p, f_d)
        d2d_copy(1, p, c).start()

    for i in range(3):
        for k in range(1, n_tp):
            frm = (t - k + n_tp) % n_tp
            dst = wts.at[i, :, pl.ds(pl.multiple_of(frm * cols, cols), cols)]
            rc(dst, dst, w_ss.at[i, frm], w_rs.at[i, frm], partner).wait_recv()

    acc[...] = jnp.zeros_like(acc)

    def core_copy(p):
        return rc(part.at[p * 2 + 1 - c], core_in.at[p], core_ss.at[p], core_rs.at[p], partner)

    def half_copy(p, first_x, i):
        q = jnp.where(first_x, i * 2 + (1 - fx), (1 - fy) * 2 + i)
        dev = {"fs": jnp.where(first_x, f_x, f_y)}
        return rc(part.at[p * 2 + c, qs(q)], half_in.at[p, i], half_ss.at[p, i], half_rs.at[p, i], dev)

    @pl.loop(0, n_z)
    def _(j):
        p = sweep(j)
        for arr in range(2):
            dst = tok.at[arr, p * 2 + 1 - c]
            rc(dst, dst, d2d_ss.at[arr, p], d2d_rs.at[arr, p], partner).wait_recv()

        @pl.loop(0, 2)
        def _(u):
            s = p * 2 + jnp.where(u == 0, 1 - c, c)
            rows, ct = tok[0, s], tok[1, s]
            gate_pre = contract_hidden(rows, wts[0])
            up_pre = contract_hidden(rows, wts[1])
            hidden_grad = contract_hidden(ct, wts[2])
            sig = jax.nn.sigmoid(gate_pre)
            silu = gate_pre * sig
            hidden = (silu * up_pre).astype(BF16)
            gate_grad = (hidden_grad * up_pre * sig * (1.0 + gate_pre * (1.0 - sig))).astype(BF16)
            up_grad = (hidden_grad * silu).astype(BF16)
            acc[...] += contract_tokens(hidden, ct)
            part[s] = (
                jnp.dot(gate_grad, wts[0], preferred_element_type=F32)
                + jnp.dot(up_grad, wts[1], preferred_element_type=F32)
            ).astype(BF16)

            @pl.when(u == 0)
            def _():
                core_copy(p).start()

        core_copy(p).wait_recv()
        s = p * 2 + c
        part[s] = (part[s].astype(F32) + core_in[p].astype(F32)).astype(BF16)
        first_x = p >= n_z // 2
        half_copy(p, first_x, 0).start()
        half_copy(p, first_x, 1).start()

    down_out[...] = acc[...].astype(BF16)

    def dn_copy(k):
        to = (t + k) % n_tp
        return rc(
            down_out.at[:, pl.ds(pl.multiple_of(to * cols, cols), cols)],
            down_in.at[pl.ds(pl.multiple_of(t * hid, hid), hid)],
            dn_ss.at[k], dn_rs.at[k], {"tp": to},
        )

    for k in range(1, n_tp):
        dn_copy(k).start()

    def quarter_copy(p, first_x):
        q = jnp.where(first_x, f_y, f_x)
        return rc(
            part.at[p * 2 + c, qs(q)], quarter_in.at[p], q_ss.at[p], q_rs.at[p],
            {"fs": jnp.where(first_x, f_y, f_x)},
        )

    def half_add(p):
        first_x = p >= n_z // 2
        s = p * 2 + c
        other = jnp.where(first_x, 1 - fy, 1 - fx)
        mine = jnp.where(first_x, fy, fx)
        for i in range(2):
            half_copy(p, first_x, i).wait_recv()
        q_other = jnp.where(first_x, f_y, f_x)
        part[s, qs(q_other)] = (
            part[s, qs(q_other)].astype(F32) + half_in[p, other].astype(F32)
        ).astype(BF16)
        quarter_copy(p, first_x).start()
        part[s, qs(f)] = (part[s, qs(f)].astype(F32) + half_in[p, mine].astype(F32)).astype(BF16)

    def chain_copy(p):
        return rc(
            part.at[p * 2 + c, qs(f)], chain_in.at[z], ch_ss.at[p], ch_rs.at[z], {"tp": p * 2 + c}
        )

    @pl.loop(0, n_z + 1)
    def _(j):
        @pl.when(j < n_z)
        def _():
            half_add(sweep(j))

        @pl.when(j > 0)
        def _():
            p = sweep(j - 1)
            quarter_copy(p, p >= n_z // 2).wait_recv()
            s = p * 2 + c
            part[s, qs(f)] = (part[s, qs(f)].astype(F32) + quarter_in[p].astype(F32)).astype(BF16)

            @pl.when(p != z)
            def _():
                chain_copy(p).start()

    @pl.loop(0, n_z)
    def _(j):
        frm = sweep(j)

        @pl.when(frm != z)
        def _():
            dst = chain_in.at[frm]
            rc(dst, dst, ch_ss.at[frm], ch_rs.at[frm], partner).wait_recv()
            part[t, qs(f)] = (part[t, qs(f)].astype(F32) + dst[...].astype(F32)).astype(BF16)

    grad_ref[0, qs(f)] = part[t, qs(f)]

    def ag_copy(i, q):
        return rc(
            part.at[t, qs(f)], grad_ref.at[0, qs(q)], ag_ss.at[i], ag_rs.at[i], (dev_x, dev_y, dev_d)[i]
        )

    for i in (2, 0, 1):
        ag_copy(i, f).start()

    down_ref[pl.ds(pl.multiple_of(t * hid, hid), hid)] = acc[:, own_cols]
    for k in range(1, n_tp):
        frm = (t - k + n_tp) % n_tp
        rows = pl.ds(pl.multiple_of(frm * hid, hid), hid)
        rc(down_in.at[rows], down_in.at[rows], dn_ss.at[k], dn_rs.at[k], partner).wait_recv()
        down_ref[rows] = down_in[rows].astype(F32)

    for i, q in enumerate((f_x, f_y, f_d)):
        ag_copy(i, q).wait_recv()

    for arr in range(2):
        for p in range(n_z):
            @pl.when((z < n_z - 1) & (p <= z))
            def _(arr=arr, p=p):
                z_copy(arr, p, 1).wait_send()

            @pl.when((z > 0) & (p >= z))
            def _(arr=arr, p=p):
                z_copy(arr, p, 0).wait_send()

            d2d_copy(arr, p, c).wait_send()

            @pl.when(p != z)
            def _(arr=arr, p=p):
                xy_copy(arr, p, 0).wait_send()
                xy_copy(arr, p, 1).wait_send()
                relay_copy(arr, p).wait_send()

    for k in range(1, n_tp):
        for i in range(3):
            w_copy(i, (t + k) % n_tp).wait_send()
        dn_copy(k).wait_send()
    for p in range(n_z):
        core_copy(p).wait_send()
        half_copy(p, p >= n_z // 2, 0).wait_send()
        half_copy(p, p >= n_z // 2, 1).wait_send()
        quarter_copy(p, p >= n_z // 2).wait_send()

        @pl.when(p != z)
        def _(p=p):
            chain_copy(p).wait_send()

    for i in range(3):
        ag_copy(i, f).wait_send()


def spread(n_tp, inputs, cotangent, gate_weight, up_weight, down_weight):
    _, n_tok, width = inputs.shape
    hid_all = gate_weight.shape[1]
    hid, cols, n_z, qr = hid_all // n_tp, width // n_tp, n_tp // 2, n_tok // 4
    dma = pltpu.SemaphoreType.DMA
    vmem = pl.BlockSpec(memory_space=pltpu.VMEM)
    anyspace = pl.BlockSpec(memory_space=pl.ANY)
    return pl.pallas_call(
        functools.partial(kernel, n_tp),
        name="spread_hidden",
        out_shape=(
            jax.ShapeDtypeStruct((1, n_tok, width), BF16),
            jax.ShapeDtypeStruct((hid_all, cols), F32),
        ),
        in_specs=[anyspace, anyspace, vmem, vmem, vmem],
        out_specs=(vmem, vmem),
        scratch_shapes=[
            pltpu.VMEM((2, n_tp, n_tok, width), BF16),
            pltpu.VMEM((n_tp, n_tok, width), BF16),
            pltpu.VMEM((n_z, n_tok, width), BF16),
            pltpu.VMEM((n_z, 2, qr, width), BF16),
            pltpu.VMEM((n_z, qr, width), BF16),
            pltpu.VMEM((n_z, qr, width), BF16),
            pltpu.VMEM((3, hid, width), BF16),
            pltpu.VMEM((hid, width), F32),
            pltpu.VMEM((hid, width), BF16),
            pltpu.VMEM((hid_all, cols), BF16),
            pltpu.VMEM((hid_all, cols), BF16),
            pltpu.VMEM((hid_all, cols), BF16),
            dma((2,)), dma((2, n_z, 4)), dma((2, n_z, 2)), dma((2, n_z, 2)), dma((2, n_z)),
            dma((2, n_z)), dma((2, n_z)), dma((3, n_tp)), dma((3, n_tp)), dma((n_z,)), dma((n_z,)),
            dma((n_z, 2)), dma((n_z, 2)), dma((n_z,)), dma((n_z,)), dma((n_z,)), dma((n_z,)),
            dma((3,)), dma((3,)), dma((n_tp,)), dma((n_tp,)),
        ],
        compiler_params=pltpu.CompilerParams(
            collective_id=0, has_side_effects=True, vmem_limit_bytes=66_000_000
        ),
    )(inputs, cotangent, gate_weight, up_weight, down_weight)


def solution(mesh):
    n_fs, n_tp = mesh.shape["fs"], mesh.shape["tp"]

    def per_device(inputs, cotangent, gate_weight, up_weight, down_weight):
        _, n_tok, width = inputs.shape
        hid_all = gate_weight.shape[1]
        n_z = n_tp // 2
        fits = (
            n_fs == 4
            and n_tp % 2 == 0
            and hid_all % (n_tp * 16) == 0
            and width % (n_tp * 128) == 0
            and n_tok % 64 == 0
            and 2 * n_tok * width * (3 * n_tp + 3 * n_z + 4) + 16 * hid_all * width < 62_000_000 * 2
        )
        if not fits:
            return gathered(inputs, cotangent, gate_weight, up_weight, down_weight)
        return spread(n_tp, inputs, cotangent, gate_weight, up_weight, down_weight)

    return jax.shard_map(
        per_device,
        mesh=mesh,
        in_specs=(
            P("tp", None, None),
            P("tp", None, None),
            P("tp", "fs"),
            P("tp", "fs"),
            P("fs", "tp"),
        ),
        out_specs=(P("tp", None, None), P("fs", "tp")),
        check_vma=False,
    )
```

```python
import functools

import jax
import jax.numpy as jnp
from jax import lax
from jax.experimental import pallas as pl
from jax.experimental.pallas import tpu as pltpu
from jax.sharding import PartitionSpec as P

MESH = pl.DeviceIdType.MESH
BF16 = jnp.bfloat16
F32 = jnp.float32


def contract_hidden(left, right):
    return lax.dot_general(left, right, (((1,), (1,)), ((), ())), preferred_element_type=F32)


def contract_tokens(left, right):
    return lax.dot_general(left, right, (((0,), (0,)), ((), ())), preferred_element_type=F32)


def gathered(inputs, cotangent, gate_weight, up_weight, down_weight):
    rows_in = inputs[0]
    rows_grad = cotangent[0]
    token_count, model_width = rows_in.shape
    gate_full = lax.all_gather(gate_weight, "tp", axis=0, tiled=True)
    up_full = lax.all_gather(up_weight, "tp", axis=0, tiled=True)
    down_tall = lax.all_gather(down_weight.T, "tp", axis=0, tiled=True)
    gate_pre = jnp.dot(rows_in, gate_full, preferred_element_type=F32)
    up_pre = jnp.dot(rows_in, up_full, preferred_element_type=F32)
    sig = jax.nn.sigmoid(gate_pre)
    hidden = (gate_pre * sig * up_pre).astype(BF16)
    hidden_grad = jnp.dot(rows_grad, down_tall, preferred_element_type=F32)
    gate_grad = (hidden_grad * up_pre * sig * (1.0 + gate_pre * (1.0 - sig))).astype(BF16)
    up_grad = (hidden_grad * gate_pre * sig).astype(BF16)
    partial_down = contract_tokens(hidden, rows_grad)
    down_grad = lax.psum_scatter(
        partial_down.astype(BF16), "tp", scatter_dimension=1, tiled=True
    ).astype(F32)
    own_sum = lax.psum_scatter(
        (contract_hidden(gate_grad, gate_full) + contract_hidden(up_grad, up_full)).astype(BF16),
        "fs",
        scatter_dimension=0,
        tiled=True,
    )
    whole_grad = lax.all_gather(own_sum, "fs", axis=0, tiled=True)
    return (whole_grad.reshape(1, token_count, model_width), down_grad)


def kernel(
    n_tp, x_ref, ct_ref, wg_ref, wu_ref, wd_ref, grad_ref, down_ref,
    tok, part, core_in, half_in, quarter_in, chain_in, wts, acc, down_out, down_in,
    gate_t, up_t, loc_sem, tok_rs, z_ss, xy_ss, dg_ss, d2d_ss, d2d_rs, w_ss, w_rs, core_ss, core_rs,
    half_ss, half_rs, q_ss, q_rs, ch_ss, ch_rs, ag_ss, ag_rs, dn_ss, dn_rs,
):
    f, t = lax.axis_index("fs"), lax.axis_index("tp")
    n_z = n_tp // 2
    z, c = t // 2, t % 2
    fy, fx = f // 2, f % 2
    f_x = fy * 2 + (1 - fx)
    f_y = (1 - fy) * 2 + fx
    f_d = (1 - fy) * 2 + (1 - fx)
    dev_x, dev_y, dev_d = {"fs": f_x}, {"fs": f_y}, {"fs": f_d}
    partner = {"tp": z * 2 + (1 - c)}
    n_tok, width = tok.shape[2], tok.shape[3]
    qr = n_tok // 4
    hid = wts.shape[1]
    cols = width // n_tp

    def plane(delta):
        return {"tp": (z + delta) * 2 + c}

    def rc(src, dst, ss, rs, dev):
        return pltpu.make_async_remote_copy(
            src_ref=src, dst_ref=dst, send_sem=ss, recv_sem=rs, device_id=dev, device_id_type=MESH
        )

    def qs(q):
        return pl.ds(pl.multiple_of(q * qr, qr), qr)

    def tokq(arr, span, q):
        return tok.at[arr, span, qs(q)]

    own = [
        pltpu.make_async_copy(x_ref.at[0], tok.at[0, t], loc_sem.at[0]),
        pltpu.make_async_copy(ct_ref.at[0], tok.at[1, t], loc_sem.at[1]),
    ]
    own_cols = pl.ds(pl.multiple_of(t * cols, cols), cols)
    for copy in own:
        copy.start()

    barrier = pltpu.get_barrier_semaphore()
    for dev in (dev_x, dev_y, dev_d):
        pl.semaphore_signal(barrier, inc=1, device_id=dev, device_id_type=MESH)
    for k in range(1, n_tp):
        pl.semaphore_signal(barrier, inc=1, device_id={"tp": (t + k) % n_tp}, device_id_type=MESH)
    pl.semaphore_wait(barrier, 3 + n_tp - 1)
    for copy in own:
        copy.wait()

    def z_copy(arr, p, d):
        src = tokq(arr, p * 2 + c, f)
        return rc(src, src, z_ss.at[arr, p, d], tok_rs.at[arr, p, f], plane(1 if d else -1))

    def xy_copy(arr, p, d):
        src = tokq(arr, p * 2 + c, f)
        return rc(src, src, xy_ss.at[arr, p, d], tok_rs.at[arr, p, f], dev_y if d else dev_x)

    def relay_copy(arr, p):
        q = f_y if arr else f_x
        src = tokq(arr, p * 2 + c, q)
        return rc(src, src, dg_ss.at[arr, p], tok_rs.at[arr, p, q], dev_x if arr else dev_y)

    def tok_wait(arr, p, q):
        dst = tokq(arr, p * 2 + c, q)
        rc(dst, dst, z_ss.at[arr, p, 0], tok_rs.at[arr, p, q], dev_x).wait_recv()

    def d2d_copy(arr, p, core):
        src = tok.at[arr, p * 2 + core]
        return rc(src, src, d2d_ss.at[arr, p], d2d_rs.at[arr, p], partner)

    def w_copy(i, to):
        return rc(
            (gate_t, up_t, wd_ref)[i].at[pl.ds(pl.multiple_of(to * hid, hid), hid)],
            wts.at[i, :, own_cols], w_ss.at[i, to], w_rs.at[i, t], {"tp": to},
        )

    def w_send(d):
        @pl.loop(2, 2 * n_z)
        def _(k):
            p = z + k // 2 if d else z - k // 2

            @pl.when((p >= 0) & (p < n_z))
            def _():
                for i in range(3):
                    w_copy(i, p * 2 + k % 2).start()

    for arr in range(2):
        for d, ok in ((1, z < n_z - 1), (0, z > 0)):
            @pl.when(ok)
            def _(arr=arr, d=d):
                z_copy(arr, z, d).start()
        d2d_copy(arr, z, c).start()

    gate_t[...] = wg_ref[...].T
    up_t[...] = wu_ref[...].T
    own_rows = pl.ds(pl.multiple_of(t * hid, hid), hid)
    for i, w in enumerate((gate_t, up_t, wd_ref)):
        wts[i, :, own_cols] = w[own_rows]

    for i in range(3):
        w_copy(i, z * 2 + 1 - c).start()

    for step in range(n_z):
        for d in (1, 0):
            p = z - step if d else z + step

            if step == 0:
                continue

            @pl.when((p >= 0) & (p < n_z))
            def _(p=p, d=d):
                for arr in range(2):
                    tok_wait(arr, p, f)

                    @pl.when(z < n_z - 1 if d else z > 0)
                    def _():
                        z_copy(arr, p, d).start()

                    xy_copy(arr, p, 0).start()
                    xy_copy(arr, p, 1).start()

        for d in (1, 0):
            @pl.when((z if d else n_z - 1 - z) == step)
            def _(d=d):
                w_send(d)

    def order(j):
        return jnp.where(z < n_z // 2, z + j, z - j + n_z) % n_z

    def sweep(j):
        return jnp.where(j % 2 == 0, n_z - 1 - j // 2, j // 2)

    @pl.loop(1, n_z)
    def _(j):
        p = order(j)
        tok_wait(0, p, f_x)
        relay_copy(0, p).start()
        tok_wait(1, p, f_y)
        relay_copy(1, p).start()

    @pl.loop(1, n_z)
    def _(j):
        p = order(j)
        tok_wait(0, p, f_y)
        tok_wait(0, p, f_d)
        d2d_copy(0, p, c).start()
        tok_wait(1, p, f_x)
        tok_wait(1, p, f_d)
        d2d_copy(1, p, c).start()

    for i in range(3):
        for k in range(1, n_tp):
            frm = (t - k + n_tp) % n_tp
            dst = wts.at[i, :, pl.ds(pl.multiple_of(frm * cols, cols), cols)]
            rc(dst, dst, w_ss.at[i, frm], w_rs.at[i, frm], partner).wait_recv()

    acc[...] = jnp.zeros_like(acc)

    def core_copy(p):
        return rc(part.at[p * 2 + 1 - c], core_in.at[p], core_ss.at[p], core_rs.at[p], partner)

    def side(first_x):
        return pl.ds(width // 2 if first_x else 0, width // 2)

    def half_copy(p, first_x, i):
        q = i * 2 + (1 - fx) if first_x else (1 - fy) * 2 + i
        return rc(
            part.at[p * 2 + c, qs(q), side(first_x)], half_in.at[p, i, :, side(first_x)],
            half_ss.at[p, i, int(first_x)], half_rs.at[p, i, int(first_x)],
            dev_x if first_x else dev_y,
        )

    @pl.loop(0, n_z)
    def _(j):
        p = sweep(j)
        for arr in range(2):
            dst = tok.at[arr, p * 2 + 1 - c]
            rc(dst, dst, d2d_ss.at[arr, p], d2d_rs.at[arr, p], partner).wait_recv()

        @pl.loop(0, 2)
        def _(u):
            s = p * 2 + jnp.where(u == 0, 1 - c, c)
            rows, ct = tok[0, s], tok[1, s]
            gate_pre = contract_hidden(rows, wts[0])
            up_pre = contract_hidden(rows, wts[1])
            hidden_grad = contract_hidden(ct, wts[2])
            sig = jax.nn.sigmoid(gate_pre)
            silu = gate_pre * sig
            hidden = (silu * up_pre).astype(BF16)
            gate_grad = (hidden_grad * up_pre * sig * (1.0 + gate_pre * (1.0 - sig))).astype(BF16)
            up_grad = (hidden_grad * silu).astype(BF16)
            acc[...] += contract_tokens(hidden, ct)
            part[s] = (
                jnp.dot(gate_grad, wts[0], preferred_element_type=F32)
                + jnp.dot(up_grad, wts[1], preferred_element_type=F32)
            ).astype(BF16)

            @pl.when(u == 0)
            def _():
                core_copy(p).start()

        core_copy(p).wait_recv()
        s = p * 2 + c
        part[s] = (part[s].astype(F32) + core_in[p].astype(F32)).astype(BF16)
        for i in range(2):
            half_copy(p, True, i).start()
            half_copy(p, False, i).start()

    down_out[...] = acc[...].astype(BF16)

    def dn_copy(k):
        to = (t + k) % n_tp
        return rc(
            down_out.at[:, pl.ds(pl.multiple_of(to * cols, cols), cols)],
            down_in.at[pl.ds(pl.multiple_of(t * hid, hid), hid)],
            dn_ss.at[k], dn_rs.at[k], {"tp": to},
        )

    for k in range(1, n_tp):
        dn_copy(k).start()

    def quarter_copy(p, first_x):
        return rc(
            part.at[p * 2 + c, qs(f_y if first_x else f_x), side(first_x)],
            quarter_in.at[p, :, side(first_x)],
            q_ss.at[p, int(first_x)], q_rs.at[p, int(first_x)], dev_y if first_x else dev_x,
        )

    def half_add(p):
        s = p * 2 + c
        for first_x in (True, False):
            mine = fy if first_x else fx
            half = side(first_x)
            for i in range(2):
                half_copy(p, first_x, i).wait_recv()
            q_other = f_y if first_x else f_x
            part[s, qs(q_other), half] = (
                part[s, qs(q_other), half].astype(F32) + half_in[p, 1 - mine, :, half].astype(F32)
            ).astype(BF16)
            quarter_copy(p, first_x).start()
            part[s, qs(f), half] = (
                part[s, qs(f), half].astype(F32) + half_in[p, mine, :, half].astype(F32)
            ).astype(BF16)

    def chain_copy(p):
        return rc(
            part.at[p * 2 + c, qs(f)], chain_in.at[z], ch_ss.at[p], ch_rs.at[z], {"tp": p * 2 + c}
        )

    @pl.loop(0, n_z + 1)
    def _(j):
        @pl.when(j < n_z)
        def _():
            half_add(sweep(j))

        @pl.when(j > 0)
        def _():
            p = sweep(j - 1)
            quarter_copy(p, True).wait_recv()
            quarter_copy(p, False).wait_recv()
            s = p * 2 + c
            part[s, qs(f)] = (part[s, qs(f)].astype(F32) + quarter_in[p].astype(F32)).astype(BF16)

            @pl.when(p != z)
            def _():
                chain_copy(p).start()

    @pl.loop(0, n_z)
    def _(j):
        frm = sweep(j)

        @pl.when(frm != z)
        def _():
            dst = chain_in.at[frm]
            rc(dst, dst, ch_ss.at[frm], ch_rs.at[frm], partner).wait_recv()
            part[t, qs(f)] = (part[t, qs(f)].astype(F32) + dst[...].astype(F32)).astype(BF16)

    grad_ref[0, qs(f)] = part[t, qs(f)]

    def ag_copy(i, q):
        return rc(
            part.at[t, qs(f)], grad_ref.at[0, qs(q)], ag_ss.at[i], ag_rs.at[i], (dev_x, dev_y, dev_d)[i]
        )

    for i in (2, 0, 1):
        ag_copy(i, f).start()

    down_ref[pl.ds(pl.multiple_of(t * hid, hid), hid)] = acc[:, own_cols]
    for k in range(1, n_tp):
        frm = (t - k + n_tp) % n_tp
        rows = pl.ds(pl.multiple_of(frm * hid, hid), hid)
        rc(down_in.at[rows], down_in.at[rows], dn_ss.at[k], dn_rs.at[k], partner).wait_recv()
        down_ref[rows] = down_in[rows].astype(F32)

    for i, q in enumerate((f_x, f_y, f_d)):
        ag_copy(i, q).wait_recv()

    for arr in range(2):
        for p in range(n_z):
            @pl.when((z < n_z - 1) & (p <= z))
            def _(arr=arr, p=p):
                z_copy(arr, p, 1).wait_send()

            @pl.when((z > 0) & (p >= z))
            def _(arr=arr, p=p):
                z_copy(arr, p, 0).wait_send()

            d2d_copy(arr, p, c).wait_send()

            @pl.when(p != z)
            def _(arr=arr, p=p):
                xy_copy(arr, p, 0).wait_send()
                xy_copy(arr, p, 1).wait_send()
                relay_copy(arr, p).wait_send()

    for k in range(1, n_tp):
        for i in range(3):
            w_copy(i, (t + k) % n_tp).wait_send()
        dn_copy(k).wait_send()
    for p in range(n_z):
        core_copy(p).wait_send()
        for first_x in (True, False):
            half_copy(p, first_x, 0).wait_send()
            half_copy(p, first_x, 1).wait_send()
            quarter_copy(p, first_x).wait_send()

        @pl.when(p != z)
        def _(p=p):
            chain_copy(p).wait_send()

    for i in range(3):
        ag_copy(i, f).wait_send()


def spread(n_tp, inputs, cotangent, gate_weight, up_weight, down_weight):
    _, n_tok, width = inputs.shape
    hid_all = gate_weight.shape[1]
    hid, cols, n_z, qr = hid_all // n_tp, width // n_tp, n_tp // 2, n_tok // 4
    dma = pltpu.SemaphoreType.DMA
    vmem = pl.BlockSpec(memory_space=pltpu.VMEM)
    anyspace = pl.BlockSpec(memory_space=pl.ANY)
    return pl.pallas_call(
        functools.partial(kernel, n_tp),
        name="spread_hidden",
        out_shape=(
            jax.ShapeDtypeStruct((1, n_tok, width), BF16),
            jax.ShapeDtypeStruct((hid_all, cols), F32),
        ),
        in_specs=[anyspace, anyspace, vmem, vmem, vmem],
        out_specs=(vmem, vmem),
        scratch_shapes=[
            pltpu.VMEM((2, n_tp, n_tok, width), BF16),
            pltpu.VMEM((n_tp, n_tok, width), BF16),
            pltpu.VMEM((n_z, n_tok, width), BF16),
            pltpu.VMEM((n_z, 2, qr, width), BF16),
            pltpu.VMEM((n_z, qr, width), BF16),
            pltpu.VMEM((n_z, qr, width), BF16),
            pltpu.VMEM((3, hid, width), BF16),
            pltpu.VMEM((hid, width), F32),
            pltpu.VMEM((hid, width), BF16),
            pltpu.VMEM((hid_all, cols), BF16),
            pltpu.VMEM((hid_all, cols), BF16),
            pltpu.VMEM((hid_all, cols), BF16),
            dma((2,)), dma((2, n_z, 4)), dma((2, n_z, 2)), dma((2, n_z, 2)), dma((2, n_z)),
            dma((2, n_z)), dma((2, n_z)), dma((3, n_tp)), dma((3, n_tp)), dma((n_z,)), dma((n_z,)),
            dma((n_z, 2, 2)), dma((n_z, 2, 2)), dma((n_z, 2)), dma((n_z, 2)), dma((n_z,)), dma((n_z,)),
            dma((3,)), dma((3,)), dma((n_tp,)), dma((n_tp,)),
        ],
        compiler_params=pltpu.CompilerParams(
            collective_id=0, has_side_effects=True, vmem_limit_bytes=66_000_000
        ),
    )(inputs, cotangent, gate_weight, up_weight, down_weight)


def solution(mesh):
    n_fs, n_tp = mesh.shape["fs"], mesh.shape["tp"]

    def per_device(inputs, cotangent, gate_weight, up_weight, down_weight):
        _, n_tok, width = inputs.shape
        hid_all = gate_weight.shape[1]
        n_z = n_tp // 2
        fits = (
            n_fs == 4
            and n_tp % 2 == 0
            and hid_all % (n_tp * 16) == 0
            and width % (n_tp * 128) == 0
            and n_tok % 64 == 0
            and 2 * n_tok * width * (3 * n_tp + 3 * n_z + 4) + 16 * hid_all * width < 62_000_000 * 2
        )
        if not fits:
            return gathered(inputs, cotangent, gate_weight, up_weight, down_weight)
        return spread(n_tp, inputs, cotangent, gate_weight, up_weight, down_weight)

    return jax.shard_map(
        per_device,
        mesh=mesh,
        in_specs=(
            P("tp", None, None),
            P("tp", None, None),
            P("tp", "fs"),
            P("tp", "fs"),
            P("fs", "tp"),
        ),
        out_specs=(P("tp", None, None), P("fs", "tp")),
        check_vma=False,
    )
```
